32 devices in a mesh: sp: 4 (over z), dp: 8 (over y, x, core).
Axes of the slice: x: 2, y: 2, z: 4, core: 2. Of those that a mesh axis runs over, the one named last changes fastest.
Arguments:
- query_rows: bfloat16 [8, 512, 1024], P('dp', 'sp'), may hold values from -5.5 to 5.5
- key_rows: bfloat16 [8, 512, 1024], P('dp', 'sp'), may hold values from -5.5 to 5.5
- value_rows: bfloat16 [8, 512, 1024], P('dp', 'sp'), may hold values from -6 to 6
- lambdas: float32 [8], replicated, may hold values from 0.3 to 0.8
- query_gain: float32 [64], replicated, may hold values from 1.1 to 8
- key_gain: float32 [64], replicated, may hold values from 1.1 to 8
- sub_gain: float32 [128], replicated, may hold values from 0.1 to 1.9
- out_weight: bfloat16 [1024, 2048], P(None, 'dp'), may hold values from -0.1875 to 0.1875
Outputs:
- attended: bfloat16 [8, 512, 2048], P('dp', 'sp')
The draws below stay inside these ranges and needn't reach their ends.
All inputs are finite; a program needn't handle non-finite values.
Results may differ from the reference program's by a relative error of at most 0.0025.
The reference program's roundings to bfloat16 on the way count: a program that leaves them out, or rounds other values in their place, can miss the bound.
Values may be sent and summed in bfloat16 or wider, within the bound.
A program may use at most 64 MiB of HBM per device.

```python
import jax
import jax.numpy as jnp
from jax import lax

D = 2048
HEADS = 8
HK = 64
HV = 128
LENGTH = 512
SEQS = 8


def key_field(key):
    full_shape = (SEQS, LENGTH, 2 * HEADS * HK)
    key_base = jnp.clip(jax.random.normal(jax.random.fold_in(key, 101), full_shape, jnp.float32), -5.0, 5.0)
    return key_base


def draw_key_rows(key, part):
    return key_field(key).astype(jnp.bfloat16)


def draw_query_rows(key, part):
    full_shape = (SEQS, LENGTH, 2 * HEADS * HK)
    drawn_rows = jnp.clip(jax.random.normal(jax.random.fold_in(key, 107), full_shape, jnp.float32), -5.0, 5.0)
    return drawn_rows.astype(jnp.bfloat16)


def draw_query_gain(key, part):
    uniform_draw = jax.random.uniform(jax.random.fold_in(key, 211), (HK,), jnp.float32)
    return 1.1 + 0.5 * uniform_draw


def draw_key_gain(key, part):
    uniform_draw = jax.random.uniform(jax.random.fold_in(key, 223), (HK,), jnp.float32)
    return 1.1 + 0.5 * uniform_draw


def block_scale(own_key, shape, split, least, top_value):
    gain, own = 1.0, jax.random.fold_in(own_key, 6)
    for dim, shards_of in split:
        steps = jnp.exp(jax.random.uniform(jax.random.fold_in(own, dim), (shards_of,), jnp.float32, least / len(split), top_value / len(split)))
        gain = gain * jnp.repeat(steps, shape[dim] // shards_of).reshape([-1 if axis == dim else 1 for axis in range(len(shape))])
    return gain


def bell_draw(own_key, dims, scale, most, shards=(), kind=jnp.bfloat16):
    array = scale * jax.random.normal(own_key, dims, jnp.float32)
    if shards:
        array = array * block_scale(own_key, dims, shards, -0.22, 0.18)
    return jnp.clip(array, -most, most).astype(kind)


def setup_inputs(seed: int = 0) -> dict:
    keys = jax.random.split(jax.random.key(seed), 9)
    return {
        "query_rows": draw_query_rows(jax.random.fold_in(keys[8], 71), 0),
        "key_rows": draw_key_rows(jax.random.fold_in(keys[8], 71), 0),
        "value_rows": bell_draw(keys[2], (SEQS, LENGTH, HEADS * HV), 1.0, 6.0, ((0, 8), (1, 4))),
        "lambdas": jnp.clip(jax.random.uniform(keys[3], (HEADS,), jnp.float32, 0.3, 0.8), 0.3, 0.8),
        "query_gain": draw_query_gain(jax.random.fold_in(keys[8], 71), 0),
        "key_gain": draw_key_gain(jax.random.fold_in(keys[8], 71), 0),
        "sub_gain": jnp.clip(1.0 + 0.18 * jax.random.normal(keys[6], (HV,), jnp.float32), 0.1, 1.9),
        "out_weight": bell_draw(keys[7], (HEADS * HV, D), (HEADS * HV) ** -0.5, 0.1875, ((1, 8),)),
    }


epsilon = 1e-06
output_scale = 0.8

def normalize(field, scaling):
    return field * lax.rsqrt(lax.optimization_barrier(jnp.mean(field * field, axis=-1, keepdims=True)) + epsilon) * scaling

def reference(query_rows, key_rows, value_rows, lambdas, query_gain, key_gain, sub_gain, out_weight):
    sequences = query_rows.shape[0]
    length = query_rows.shape[1]
    groups = 2 * HEADS
    query_norm = normalize(query_rows.reshape(sequences, length, groups, HK).astype(jnp.float32), query_gain).astype(jnp.bfloat16)
    key_norm = normalize(key_rows.reshape(sequences, length, groups, HK).astype(jnp.float32), key_gain).astype(jnp.bfloat16)
    value_heads = value_rows.reshape(sequences, length, HEADS, HV)
    value_groups = jnp.concatenate([value_heads, value_heads], axis=2)
    positions = jnp.arange(length)
    causal = positions[None, :] <= positions[:, None]

    def one_group(inputs):
        group_query, group_key, group_value = inputs
        scores = jnp.dot(group_query, group_key.T, preferred_element_type=jnp.float32) * HK ** (-0.5)
        scores = jnp.where(causal, scores, -jnp.inf)
        weights = jax.nn.softmax(scores, axis=-1).astype(jnp.bfloat16)
        return jnp.dot(weights, group_value, preferred_element_type=jnp.float32).astype(jnp.bfloat16)

    def by_group(field):
        return jnp.transpose(field, (0, 2, 1, 3)).reshape(sequences * groups, length, field.shape[3])
    map_outputs = lax.map(one_group, (by_group(query_norm), by_group(key_norm), by_group(value_groups)))
    map_outputs = jnp.transpose(map_outputs.reshape(sequences, groups, length, HV), (0, 2, 1, 3)).astype(jnp.float32)
    mixed_heads = map_outputs[:, :, :HEADS] - lambdas[:, None] * map_outputs[:, :, HEADS:]
    normed = (normalize(mixed_heads, sub_gain) * output_scale).astype(jnp.bfloat16).reshape(sequences * length, HEADS * HV)
    projected = jnp.dot(normed, out_weight, preferred_element_type=jnp.float32)
    return projected.astype(jnp.bfloat16).reshape(sequences, length, D)
```

```python
import functools

import jax
import jax.numpy as jnp
from jax import lax
from jax.experimental import pallas as pl
from jax.experimental.pallas import tpu as pltpu
from jax.sharding import PartitionSpec as P

D = 2048
HEADS = 8
HK = 64
HV = 128


epsilon = 1e-06
output_scale = 0.8


def normalize(field, scaling):
    return field * lax.rsqrt(jnp.mean(field * field, axis=-1, keepdims=True) + epsilon) * scaling


def attend(arrived, length):
    block_rows = max(min(512, length), length // 16)
    results = []
    for number in range(length // block_rows):
        first_row = number * block_rows
        last_row = first_row + block_rows
        query_block = arrived[first_row:last_row, :, :HK]
        key_block = arrived[:last_row, :, HK : 2 * HK]
        value_block = arrived[:last_row, :, 2 * HK :]
        scores = jnp.einsum(
            "qgd,kgd->gqk", query_block, key_block, preferred_element_type=jnp.float32
        ) * HK ** (-0.5)
        visible = jnp.arange(last_row)[None, :] <= (first_row + jnp.arange(block_rows))[:, None]
        scores = jnp.where(visible[None], scores, -jnp.inf)
        weights = jax.nn.softmax(scores, axis=-1).astype(jnp.bfloat16)
        results.append(
            jnp.einsum(
                "gqk,kgd->qgd", weights, value_block, preferred_element_type=jnp.float32
            ).astype(jnp.bfloat16)
        )
    return jnp.concatenate(results, axis=0)


def body(query_rows, key_rows, value_rows, lambdas, query_gain, key_gain, sub_gain, out_weight):
    sequences = query_rows.shape[0]
    tokens_here = query_rows.shape[1]
    groups = 2 * HEADS
    query_norm = normalize(
        query_rows.reshape(sequences, tokens_here, groups, HK).astype(jnp.float32), query_gain
    ).astype(jnp.bfloat16)
    key_norm = normalize(
        key_rows.reshape(sequences, tokens_here, groups, HK).astype(jnp.float32), key_gain
    ).astype(jnp.bfloat16)
    value_heads = value_rows.reshape(sequences, tokens_here, HEADS, HV)
    packet = jnp.concatenate(
        [query_norm, key_norm, jnp.concatenate([value_heads, value_heads], axis=2)], axis=3
    )
    arrived = lax.all_to_all(packet, "sp", split_axis=2, concat_axis=1, tiled=True)
    length = arrived.shape[1]
    map_outputs = attend(arrived[0], length)[None]
    returned = lax.all_to_all(map_outputs, "sp", split_axis=1, concat_axis=2, tiled=True)
    returned_float = returned.astype(jnp.float32)
    mixed_heads = returned_float[:, :, :HEADS] - lambdas[:, None] * returned_float[:, :, HEADS:]
    normed = (
        (normalize(mixed_heads, sub_gain) * output_scale)
        .astype(jnp.bfloat16)
        .reshape(sequences * tokens_here, HEADS * HV)
    )
    projected = jnp.dot(
        normed,
        lax.all_gather(out_weight, "dp", axis=1, tiled=True),
        preferred_element_type=jnp.float32,
    )
    return projected.astype(jnp.bfloat16).reshape(sequences, tokens_here, D)


MESH = pl.DeviceIdType.MESH


def fits(sp, dp, rows_shape, weight_shape):
    if HEADS % sp or (HEADS // sp * HK) % 128 or dp % 2:
        return False
    return rows_shape[0] == 1 and rows_shape[1] % 128 == 0 and rows_shape[1] * sp <= 1024 and weight_shape[1] % 128 == 0


def kernel(
    sp, dp, q_ref, k_ref, v_ref, lam_ref, qg_ref, kg_ref, sg_ref, w_ref, out_ref,
    qb, kb, vb, kn, first, nsend, nbuf, wbuf,
    in_send, in_recv, back_send, back_recv, w_send, w_recv, p_send, p_recv,
):
    me, d = lax.axis_index("sp"), lax.axis_index("dp")
    partner = d + 1 - 2 * lax.rem(d, 2)
    chips = dp // 2
    rows = q_ref.shape[0]
    local = HEADS // sp
    width, vwidth = local * HK, local * HV
    columns = w_ref.shape[1]

    barrier = pltpu.get_barrier_semaphore()
    for o in range(1, sp):
        pl.semaphore_signal(barrier, inc=1, device_id=(lax.rem(me + o, sp), d), device_id_type=MESH)
    for c in range(1, chips):
        pl.semaphore_signal(barrier, inc=1, device_id=(me, lax.rem(d + 2 * c, dp)), device_id_type=MESH)
    pl.semaphore_signal(barrier, inc=1, device_id=(me, partner), device_id_type=MESH)
    pl.semaphore_wait(barrier, sp - 1 + chips)

    def span(i):
        return pl.ds(pl.multiple_of(i * rows, rows), rows)

    def pieces(target, source):
        low = pl.ds(pl.multiple_of(target * width, 128), width)
        high = pl.ds(pl.multiple_of(HEADS * HK + target * width, 128), width)
        vals = pl.ds(pl.multiple_of(target * vwidth, 128), vwidth)
        there = span(source)
        return (
            (k_ref.at[:, low], kb.at[0, there, :]),
            (q_ref.at[:, low], qb.at[0, there, :]),
            (v_ref.at[:, vals], vb.at[there, :]),
            (k_ref.at[:, high], kb.at[1, there, :]),
            (q_ref.at[:, high], qb.at[1, there, :]),
        )

    def forward(o, t):
        target = lax.rem(me + o, sp)
        src, dst = pieces(target, me)[t]
        return pltpu.make_async_remote_copy(
            src_ref=src, dst_ref=dst, send_sem=in_send.at[o, t], recv_sem=in_recv.at[me, t],
            device_id=(target, d), device_id_type=MESH,
        )

    def mine(t):
        src, dst = pieces(me, me)[t]
        return pltpu.make_async_copy(src, dst, in_recv.at[me, t])

    def arrived(i, t):
        @pl.when(i == me)
        def _():
            mine(t).wait()

        @pl.when(i != me)
        def _():
            src, dst = pieces(me, i)[t]
            pltpu.make_async_remote_copy(
                src_ref=src, dst_ref=dst, send_sem=in_send.at[0, t], recv_sem=in_recv.at[i, t],
                device_id=(me, d), device_id_type=MESH,
            ).wait_recv()

    def spread(c):
        return pltpu.make_async_remote_copy(
            src_ref=w_ref, dst_ref=wbuf.at[d], send_sem=w_send.at[c], recv_sem=w_recv.at[c],
            device_id=(me, lax.rem(d + 2 * c, dp)), device_id_type=MESH,
        )

    def shard_of(device, c):
        return lax.rem(device - 2 * c + dp, dp)

    def pair(c):
        at = shard_of(d, c)
        return pltpu.make_async_remote_copy(
            src_ref=w_ref if c == 0 else wbuf.at[at], dst_ref=wbuf.at[at],
            send_sem=p_send.at[c], recv_sem=p_recv.at[c],
            device_id=(me, partner), device_id_type=MESH,
        )

    def back(i):
        return pltpu.make_async_remote_copy(
            src_ref=nsend.at[i], dst_ref=nbuf.at[me], send_sem=back_send.at[i], recv_sem=back_recv.at[me],
            device_id=(i, d), device_id_type=MESH,
        )

    for t in range(5):
        mine(t).start()
        for o in range(1, sp):
            forward(o, t).start()
        if t == 0:
            for c in range(1, chips):
                spread(c).start()
            pair(0).start()

    lane = lax.broadcasted_iota(jnp.int32, (width, width), 1) // HK
    ones = (lane == lax.broadcasted_iota(jnp.int32, (width, width), 0) // HK).astype(jnp.bfloat16)
    head_of = lax.broadcasted_iota(jnp.int32, (rows, width), 1) // HK
    visible = lax.broadcasted_iota(jnp.int32, (rows, rows), 1) <= lax.broadcasted_iota(jnp.int32, (rows, rows), 0)
    visible = jnp.concatenate([visible] * local, axis=0)
    query_gain = jnp.concatenate([qg_ref[...]] * local, axis=1)
    key_gain = jnp.concatenate([kg_ref[...]] * local, axis=1)
    sub_gain = sg_ref[...] * output_scale

    def normed_rows(block, gain):
        field = block.astype(jnp.float32)
        square = field * field
        upper = square.astype(jnp.bfloat16)
        lower = (square - upper.astype(jnp.float32)).astype(jnp.bfloat16)
        total = jnp.dot(upper, ones, preferred_element_type=jnp.float32)
        total += jnp.dot(lower, ones, preferred_element_type=jnp.float32)
        return (field * lax.rsqrt(total * (1.0 / HK) + epsilon) * gain).astype(jnp.bfloat16)

    def attend_block(m, i):
        base, keys = i * rows, (i + 1) * rows
        kn[m, base:keys, :] = normed_rows(kb[m, base:keys, :], key_gain)
        query = normed_rows(qb[m, base:keys, :], query_gain)
        zero = jnp.zeros_like(query)
        stacked = jnp.concatenate([jnp.where(head_of == h, query, zero) for h in range(local)], axis=0)
        scores = lax.dot_general(
            stacked, kn[m, :keys, :], (((1,), (1,)), ((), ())), preferred_element_type=jnp.float32
        ) * HK ** (-0.5)
        last = jnp.where(visible, scores[:, base:], -jnp.inf)
        scores = last if i == 0 else jnp.concatenate([scores[:, :base], last], axis=1)
        raised = jnp.exp(scores - jnp.max(scores, axis=1, keepdims=True))
        weights = (raised * (1.0 / jnp.sum(raised, axis=1, keepdims=True))).astype(jnp.bfloat16)
        return [
            jnp.dot(
                weights[h * rows : (h + 1) * rows], vb[:keys, h * HV : (h + 1) * HV],
                preferred_element_type=jnp.float32,
            ).astype(jnp.bfloat16)
            for h in range(local)
        ]

    for i in range(sp):
        for t in range(3):
            arrived(i, t)
        for h, part in enumerate(attend_block(0, i)):
            first[i * rows : (i + 1) * rows, h * HV : (h + 1) * HV] = part

    for i in range(sp):
        for t in range(3, 5):
            arrived(i, t)
        for h, part in enumerate(attend_block(1, i)):
            before = first[i * rows : (i + 1) * rows, h * HV : (h + 1) * HV].astype(jnp.float32)
            mixed = before - lam_ref[me * local + h] * part.astype(jnp.float32)
            mean = jnp.mean(mixed * mixed, axis=1, keepdims=True)
            nsend[i, :, h * HV : (h + 1) * HV] = (mixed * lax.rsqrt(mean + epsilon) * sub_gain).astype(jnp.bfloat16)

        @pl.when(i == me)
        def _():
            nbuf[i] = nsend[i]

        @pl.when(i != me)
        def _():
            back(i).start()

    for c in range(1, chips):
        spread(c).wait_recv()
        pair(c).start()

    for i in range(sp):
        @pl.when(i != me)
        def _():
            pltpu.make_async_remote_copy(
                src_ref=nsend.at[i], dst_ref=nbuf.at[i], send_sem=back_send.at[i], recv_sem=back_recv.at[i],
                device_id=(i, d), device_id_type=MESH,
            ).wait_recv()

    normed = jnp.concatenate([nbuf[j] for j in range(sp)], axis=1)

    def project(shard, weight):
        out_ref[:, pl.ds(pl.multiple_of(shard * columns, 128), columns)] = jnp.dot(
            normed, weight, preferred_element_type=jnp.float32
        ).astype(jnp.bfloat16)

    project(d, w_ref[...])
    for c in range(1, chips):
        project(shard_of(d, c), wbuf[shard_of(d, c)])
    for c in range(chips):
        at = shard_of(partner, c)
        pltpu.make_async_remote_copy(
            src_ref=w_ref, dst_ref=wbuf.at[at], send_sem=p_send.at[c], recv_sem=p_recv.at[c],
            device_id=(me, partner), device_id_type=MESH,
        ).wait_recv()
        project(at, wbuf[at])

    for o in range(1, sp):
        for t in range(5):
            forward(o, t).wait_send()
    for c in range(chips):
        pair(c).wait_send()
        if c:
            spread(c).wait_send()
    for i in range(sp):
        @pl.when(i != me)
        def _():
            back(i).wait_send()


def fused(sp, dp, query_rows, key_rows, value_rows, lambdas, query_gain, key_gain, sub_gain, out_weight):
    rows = query_rows.shape[1]
    length = rows * sp
    local = HEADS // sp
    width, vwidth = local * HK, local * HV
    depth, columns = out_weight.shape
    vmem = pl.BlockSpec(memory_space=pltpu.VMEM)
    dma = pltpu.SemaphoreType.DMA
    out = pl.pallas_call(
        functools.partial(kernel, sp, dp),
        out_shape=jax.ShapeDtypeStruct((rows, columns * dp), jnp.bfloat16),
        in_specs=[vmem] * 3 + [pl.BlockSpec(memory_space=pltpu.SMEM)] + [vmem] * 4,
        out_specs=vmem,
        scratch_shapes=[
            pltpu.VMEM((2, length, width), jnp.bfloat16),
            pltpu.VMEM((2, length, width), jnp.bfloat16),
            pltpu.VMEM((length, vwidth), jnp.bfloat16),
            pltpu.VMEM((2, length, width), jnp.bfloat16),
            pltpu.VMEM((length, vwidth), jnp.bfloat16),
            pltpu.VMEM((sp, rows, vwidth), jnp.bfloat16),
            pltpu.VMEM((sp, rows, vwidth), jnp.bfloat16),
            pltpu.VMEM((dp, depth, columns), jnp.bfloat16),
            dma((sp, 5)), dma((sp, 5)), dma((sp,)), dma((sp,)),
            dma((dp // 2,)), dma((dp // 2,)), dma((dp // 2,)), dma((dp // 2,)),
        ],
        compiler_params=pltpu.CompilerParams(collective_id=0, has_side_effects=True),
    )(
        query_rows[0], key_rows[0], value_rows[0], lambdas,
        query_gain[None], key_gain[None], sub_gain[None], out_weight,
    )
    return out[None]


def solution(mesh):
    in_specs = (
        P("dp", "sp", None),
        P("dp", "sp", None),
        P("dp", "sp", None),
        P(),
        P(),
        P(),
        P(),
        P(None, "dp"),
    )
    out_specs = P("dp", "sp", None)
    sp, dp = mesh.shape["sp"], mesh.shape["dp"]

    def step(*operands):
        if fits(sp, dp, operands[0].shape, operands[7].shape):
            return fused(sp, dp, *operands)
        return body(*operands)

    return jax.shard_map(step, mesh=mesh, in_specs=in_specs, out_specs=out_specs, check_vma=False)
```

```python
import functools

import jax
import jax.numpy as jnp
from jax import lax
from jax.experimental import pallas as pl
from jax.experimental.pallas import tpu as pltpu
from jax.sharding import PartitionSpec as P

D = 2048
HEADS = 8
HK = 64
HV = 128


epsilon = 1e-06
output_scale = 0.8


def normalize(field, scaling):
    return field * lax.rsqrt(jnp.mean(field * field, axis=-1, keepdims=True) + epsilon) * scaling


def attend(arrived, length):
    block_rows = max(min(512, length), length // 16)
    results = []
    for number in range(length // block_rows):
        first_row = number * block_rows
        last_row = first_row + block_rows
        query_block = arrived[first_row:last_row, :, :HK]
        key_block = arrived[:last_row, :, HK : 2 * HK]
        value_block = arrived[:last_row, :, 2 * HK :]
        scores = jnp.einsum(
            "qgd,kgd->gqk", query_block, key_block, preferred_element_type=jnp.float32
        ) * HK ** (-0.5)
        visible = jnp.arange(last_row)[None, :] <= (first_row + jnp.arange(block_rows))[:, None]
        scores = jnp.where(visible[None], scores, -jnp.inf)
        weights = jax.nn.softmax(scores, axis=-1).astype(jnp.bfloat16)
        results.append(
            jnp.einsum(
                "gqk,kgd->qgd", weights, value_block, preferred_element_type=jnp.float32
            ).astype(jnp.bfloat16)
        )
    return jnp.concatenate(results, axis=0)


def body(query_rows, key_rows, value_rows, lambdas, query_gain, key_gain, sub_gain, out_weight):
    sequences = query_rows.shape[0]
    tokens_here = query_rows.shape[1]
    groups = 2 * HEADS
    query_norm = normalize(
        query_rows.reshape(sequences, tokens_here, groups, HK).astype(jnp.float32), query_gain
    ).astype(jnp.bfloat16)
    key_norm = normalize(
        key_rows.reshape(sequences, tokens_here, groups, HK).astype(jnp.float32), key_gain
    ).astype(jnp.bfloat16)
    value_heads = value_rows.reshape(sequences, tokens_here, HEADS, HV)
    packet = jnp.concatenate(
        [query_norm, key_norm, jnp.concatenate([value_heads, value_heads], axis=2)], axis=3
    )
    arrived = lax.all_to_all(packet, "sp", split_axis=2, concat_axis=1, tiled=True)
    length = arrived.shape[1]
    map_outputs = attend(arrived[0], length)[None]
    returned = lax.all_to_all(map_outputs, "sp", split_axis=1, concat_axis=2, tiled=True)
    returned_float = returned.astype(jnp.float32)
    mixed_heads = returned_float[:, :, :HEADS] - lambdas[:, None] * returned_float[:, :, HEADS:]
    normed = (
        (normalize(mixed_heads, sub_gain) * output_scale)
        .astype(jnp.bfloat16)
        .reshape(sequences * tokens_here, HEADS * HV)
    )
    projected = jnp.dot(
        normed,
        lax.all_gather(out_weight, "dp", axis=1, tiled=True),
        preferred_element_type=jnp.float32,
    )
    return projected.astype(jnp.bfloat16).reshape(sequences, tokens_here, D)


MESH = pl.DeviceIdType.MESH


def fits(sp, dp, rows_shape, weight_shape):
    if HEADS % sp or (HEADS // sp * HK) % 128 or dp % 2:
        return False
    return rows_shape[0] == 1 and rows_shape[1] % 128 == 0 and rows_shape[1] * sp <= 1024 and weight_shape[1] % 128 == 0


def kernel(
    sp, dp, q_ref, k_ref, v_ref, lam_ref, qg_ref, kg_ref, sg_ref, w_ref, out_ref,
    qb, kb, vb, kn, first, nsend, nbuf, wbuf,
    in_send, in_recv, back_send, back_recv, w_send, w_recv, p_send, p_recv, own_sem,
):
    me, d = lax.axis_index("sp"), lax.axis_index("dp")
    partner = d + 1 - 2 * lax.rem(d, 2)
    chips = dp // 2
    rows = q_ref.shape[0]
    local = HEADS // sp
    width, vwidth = local * HK, local * HV
    depth, columns = w_ref.shape
    half = depth // 2
    square = chips == 4

    def fellow(c, device=d):
        if not square:
            return lax.rem(device + 2 * c, dp)
        core, chip = lax.rem(device, 2), device // 2
        x, y = lax.rem(chip, 2), chip // 2
        x = 1 - x if c % 2 else x
        y = 1 - y if c // 2 else y
        return (y * 2 + x) * 2 + core

    barrier = pltpu.get_barrier_semaphore()
    for o in range(1, sp):
        pl.semaphore_signal(barrier, inc=1, device_id=(lax.rem(me + o, sp), d), device_id_type=MESH)
    for c in range(1, chips):
        pl.semaphore_signal(barrier, inc=1, device_id=(me, fellow(c)), device_id_type=MESH)
    pl.semaphore_signal(barrier, inc=1, device_id=(me, partner), device_id_type=MESH)
    pl.semaphore_wait(barrier, sp - 1 + chips)

    def span(i):
        return pl.ds(pl.multiple_of(i * rows, rows), rows)

    def pieces(target, source):
        low = pl.ds(pl.multiple_of(target * width, 128), width)
        high = pl.ds(pl.multiple_of(HEADS * HK + target * width, 128), width)
        vals = pl.ds(pl.multiple_of(target * vwidth, 128), vwidth)
        there = span(source)
        return (
            (k_ref.at[:, low], kb.at[0, there, :]),
            (q_ref.at[:, low], qb.at[0, there, :]),
            (v_ref.at[:, vals], vb.at[there, :]),
            (k_ref.at[:, high], kb.at[1, there, :]),
            (q_ref.at[:, high], qb.at[1, there, :]),
        )

    def forward(o, t):
        target = lax.rem(me + o, sp)
        src, dst = pieces(target, me)[t]
        return pltpu.make_async_remote_copy(
            src_ref=src, dst_ref=dst, send_sem=in_send.at[o, t], recv_sem=in_recv.at[me, t],
            device_id=(target, d), device_id_type=MESH,
        )

    def mine(t):
        src, dst = pieces(me, me)[t]
        return pltpu.make_async_copy(src, dst, in_recv.at[me, t])

    def arrived(i, t):
        @pl.when(i == me)
        def _():
            mine(t).wait()

        @pl.when(i != me)
        def _():
            src, dst = pieces(me, i)[t]
            pltpu.make_async_remote_copy(
                src_ref=src, dst_ref=dst, send_sem=in_send.at[0, t], recv_sem=in_recv.at[i, t],
                device_id=(me, d), device_id_type=MESH,
            ).wait_recv()

    def rows_of(h):
        return pl.ds(h * half, half)

    def spread(c, h):
        source, over = d, c
        if square and c == 3:
            source, over = fellow(1 + h), 2 - h
        src = w_ref if source is d else wbuf.at[source]
        return pltpu.make_async_remote_copy(
            src_ref=src.at[rows_of(h)], dst_ref=wbuf.at[source, rows_of(h)], send_sem=w_send.at[c, h], recv_sem=w_recv.at[c, h],
            device_id=(me, fellow(over)), device_id_type=MESH,
        )

    def shard_of(device, c):
        if c == 0:
            return device
        return fellow(c, device) if square else lax.rem(device - 2 * c + dp, dp)

    def own_weights():
        return pltpu.make_async_copy(w_ref, wbuf.at[d], own_sem)

    def gained(c, h):
        at = shard_of(d, c)
        pltpu.make_async_remote_copy(
            src_ref=wbuf.at[at, rows_of(h)], dst_ref=wbuf.at[at, rows_of(h)], send_sem=w_send.at[c, h], recv_sem=w_recv.at[c, h],
            device_id=(me, partner), device_id_type=MESH,
        ).wait_recv()

    def pair(c):
        at = shard_of(d, c)
        return pltpu.make_async_remote_copy(
            src_ref=w_ref if c == 0 else wbuf.at[at], dst_ref=wbuf.at[at],
            send_sem=p_send.at[c], recv_sem=p_recv.at[c],
            device_id=(me, partner), device_id_type=MESH,
        )

    def back(i):
        return pltpu.make_async_remote_copy(
            src_ref=nsend.at[i], dst_ref=nbuf.at[me], send_sem=back_send.at[i], recv_sem=back_recv.at[me],
            device_id=(i, d), device_id_type=MESH,
        )

    for t in range(5):
        mine(t).start()
        for o in range(1, sp):
            forward(o, t).start()
        if t == 0:
            for order in range(2):
                for c in range(1, chips):
                    if not (square and c == 3):
                        spread(c, (c + 1 + order) % 2).start()
            pair(0).start()
            own_weights().start()
    if square:
        for h in range(2):
            gained(1 + h, h)
            spread(3, h).start()

    lane = lax.broadcasted_iota(jnp.int32, (width, width), 1) // HK
    ones = (lane == lax.broadcasted_iota(jnp.int32, (width, width), 0) // HK).astype(jnp.bfloat16)
    head_of = lax.broadcasted_iota(jnp.int32, (rows, width), 1) // HK
    visible = lax.broadcasted_iota(jnp.int32, (rows, rows), 1) <= lax.broadcasted_iota(jnp.int32, (rows, rows), 0)
    visible = jnp.concatenate([visible] * local, axis=0)
    query_gain = jnp.concatenate([qg_ref[...]] * local, axis=1)
    key_gain = jnp.concatenate([kg_ref[...]] * local, axis=1)
    sub_gain = sg_ref[...] * output_scale

    def normed_rows(block, gain):
        field = block.astype(jnp.float32)
        square = field * field
        upper = square.astype(jnp.bfloat16)
        lower = (square - upper.astype(jnp.float32)).astype(jnp.bfloat16)
        total = jnp.dot(upper, ones, preferred_element_type=jnp.float32)
        total += jnp.dot(lower, ones, preferred_element_type=jnp.float32)
        return (field * lax.rsqrt(total * (1.0 / HK) + epsilon) * gain).astype(jnp.bfloat16)

    def attend_block(m, i):
        base, keys = i * rows, (i + 1) * rows
        kn[m, base:keys, :] = normed_rows(kb[m, base:keys, :], key_gain)
        query = normed_rows(qb[m, base:keys, :], query_gain)
        zero = jnp.zeros_like(query)
        stacked = jnp.concatenate([jnp.where(head_of == h, query, zero) for h in range(local)], axis=0)
        scores = lax.dot_general(
            stacked, kn[m, :keys, :], (((1,), (1,)), ((), ())), preferred_element_type=jnp.float32
        ) * HK ** (-0.5)
        last = jnp.where(visible, scores[:, base:], -jnp.inf)
        scores = last if i == 0 else jnp.concatenate([scores[:, :base], last], axis=1)
        raised = jnp.exp(scores - jnp.max(scores, axis=1, keepdims=True))
        weights = (raised * (1.0 / jnp.sum(raised, axis=1, keepdims=True))).astype(jnp.bfloat16)
        return [
            jnp.dot(
                weights[h * rows : (h + 1) * rows], vb[:keys, h * HV : (h + 1) * HV],
                preferred_element_type=jnp.float32,
            ).astype(jnp.bfloat16)
            for h in range(local)
        ]

    for i in range(sp):
        for t in range(3):
            arrived(i, t)
        for h, part in enumerate(attend_block(0, i)):
            first[i * rows : (i + 1) * rows, h * HV : (h + 1) * HV] = part

    if square:
        for h in range(2):
            gained(1 + h, 1 - h)
            pair(1 + h).start()

    for i in range(sp):
        for t in range(3, 5):
            arrived(i, t)
        for h, part in enumerate(attend_block(1, i)):
            before = first[i * rows : (i + 1) * rows, h * HV : (h + 1) * HV].astype(jnp.float32)
            mixed = before - lam_ref[me * local + h] * part.astype(jnp.float32)
            mean = jnp.mean(mixed * mixed, axis=1, keepdims=True)
            nsend[i, :, h * HV : (h + 1) * HV] = (mixed * lax.rsqrt(mean + epsilon) * sub_gain).astype(jnp.bfloat16)

        @pl.when(i == me)
        def _():
            nbuf[i] = nsend[i]

        @pl.when(i != me)
        def _():
            back(i).start()

    for c in range(3 if square else 1, chips):
        for h in range(2):
            gained(c, h)
        pair(c).start()

    for i in range(sp):
        @pl.when(i != me)
        def _():
            pltpu.make_async_remote_copy(
                src_ref=nsend.at[i], dst_ref=nbuf.at[i], send_sem=back_send.at[i], recv_sem=back_recv.at[i],
                device_id=(i, d), device_id_type=MESH,
            ).wait_recv()

    normed = jnp.concatenate([nbuf[j] for j in range(sp)], axis=1)

    def project(shard, weight):
        out_ref[:, pl.ds(pl.multiple_of(shard * columns, 128), columns)] = jnp.dot(
            normed, weight, preferred_element_type=jnp.float32
        ).astype(jnp.bfloat16)

    own_weights().wait()
    for c in range(chips):
        project(shard_of(d, c), wbuf[shard_of(d, c)])
    for c in range(chips):
        at = shard_of(partner, c)
        pltpu.make_async_remote_copy(
            src_ref=wbuf.at[at], dst_ref=wbuf.at[at], send_sem=p_send.at[c], recv_sem=p_recv.at[c],
            device_id=(me, partner), device_id_type=MESH,
        ).wait_recv()
        project(at, wbuf[at])

    for o in range(1, sp):
        for t in range(5):
            forward(o, t).wait_send()
    for c in range(chips):
        pair(c).wait_send()
        if c:
            for h in range(2):
                spread(c, h).wait_send()
    for i in range(sp):
        @pl.when(i != me)
        def _():
            back(i).wait_send()


def fused(sp, dp, query_rows, key_rows, value_rows, lambdas, query_gain, key_gain, sub_gain, out_weight):
    rows = query_rows.shape[1]
    length = rows * sp
    local = HEADS // sp
    width, vwidth = local * HK, local * HV
    depth, columns = out_weight.shape
    vmem = pl.BlockSpec(memory_space=pltpu.VMEM)
    hbm = pl.BlockSpec(memory_space=pl.ANY)
    dma = pltpu.SemaphoreType.DMA
    out = pl.pallas_call(
        functools.partial(kernel, sp, dp),
        out_shape=pltpu.VMEM((rows, columns * dp), jnp.bfloat16),
        in_specs=[hbm] * 3 + [pl.BlockSpec(memory_space=pltpu.SMEM)] + [vmem] * 3 + [hbm],
        out_specs=vmem,
        scratch_shapes=[
            pltpu.VMEM((2, length, width), jnp.bfloat16),
            pltpu.VMEM((2, length, width), jnp.bfloat16),
            pltpu.VMEM((length, vwidth), jnp.bfloat16),
            pltpu.VMEM((2, length, width), jnp.bfloat16),
            pltpu.VMEM((length, vwidth), jnp.bfloat16),
            pltpu.VMEM((sp, rows, vwidth), jnp.bfloat16),
            pltpu.VMEM((sp, rows, vwidth), jnp.bfloat16),
            pltpu.VMEM((dp, depth, columns), jnp.bfloat16),
            dma((sp, 5)), dma((sp, 5)), dma((sp,)), dma((sp,)),
            dma((dp // 2, 2)), dma((dp // 2, 2)), dma((dp // 2,)), dma((dp // 2,)), dma,
        ],
        compiler_params=pltpu.CompilerParams(collective_id=0, has_side_effects=True),
    )(
        query_rows[0], key_rows[0], value_rows[0], lambdas,
        query_gain[None], key_gain[None], sub_gain[None], out_weight,
    )
    return out[None]


def solution(mesh):
    in_specs = (
        P("dp", "sp", None),
        P("dp", "sp", None),
        P("dp", "sp", None),
        P(),
        P(),
        P(),
        P(),
        P(None, "dp"),
    )
    out_specs = P("dp", "sp", None)
    sp, dp = mesh.shape["sp"], mesh.shape["dp"]

    def step(*operands):
        if fits(sp, dp, operands[0].shape, operands[7].shape):
            return fused(sp, dp, *operands)
        return body(*operands)

    return jax.shard_map(step, mesh=mesh, in_specs=in_specs, out_specs=out_specs, check_vma=False)
```

```python
import functools

import jax
import jax.numpy as jnp
from jax import lax
from jax.experimental import pallas as pl
from jax.experimental.pallas import tpu as pltpu
from jax.sharding import PartitionSpec as P

D = 2048
HEADS = 8
HK = 64
HV = 128


epsilon = 1e-06
output_scale = 0.8


def normalize(field, scaling):
    return field * lax.rsqrt(jnp.mean(field * field, axis=-1, keepdims=True) + epsilon) * scaling


def attend(arrived, length):
    block_rows = max(min(512, length), length // 16)
    results = []
    for number in range(length // block_rows):
        first_row = number * block_rows
        last_row = first_row + block_rows
        query_block = arrived[first_row:last_row, :, :HK]
        key_block = arrived[:last_row, :, HK : 2 * HK]
        value_block = arrived[:last_row, :, 2 * HK :]
        scores = jnp.einsum(
            "qgd,kgd->gqk", query_block, key_block, preferred_element_type=jnp.float32
        ) * HK ** (-0.5)
        visible = jnp.arange(last_row)[None, :] <= (first_row + jnp.arange(block_rows))[:, None]
        scores = jnp.where(visible[None], scores, -jnp.inf)
        weights = jax.nn.softmax(scores, axis=-1).astype(jnp.bfloat16)
        results.append(
            jnp.einsum(
                "gqk,kgd->qgd", weights, value_block, preferred_element_type=jnp.float32
            ).astype(jnp.bfloat16)
        )
    return jnp.concatenate(results, axis=0)


def body(query_rows, key_rows, value_rows, lambdas, query_gain, key_gain, sub_gain, out_weight):
    sequences = query_rows.shape[0]
    tokens_here = query_rows.shape[1]
    groups = 2 * HEADS
    query_norm = normalize(
        query_rows.reshape(sequences, tokens_here, groups, HK).astype(jnp.float32), query_gain
    ).astype(jnp.bfloat16)
    key_norm = normalize(
        key_rows.reshape(sequences, tokens_here, groups, HK).astype(jnp.float32), key_gain
    ).astype(jnp.bfloat16)
    value_heads = value_rows.reshape(sequences, tokens_here, HEADS, HV)
    packet = jnp.concatenate(
        [query_norm, key_norm, jnp.concatenate([value_heads, value_heads], axis=2)], axis=3
    )
    arrived = lax.all_to_all(packet, "sp", split_axis=2, concat_axis=1, tiled=True)
    length = arrived.shape[1]
    map_outputs = attend(arrived[0], length)[None]
    returned = lax.all_to_all(map_outputs, "sp", split_axis=1, concat_axis=2, tiled=True)
    returned_float = returned.astype(jnp.float32)
    mixed_heads = returned_float[:, :, :HEADS] - lambdas[:, None] * returned_float[:, :, HEADS:]
    normed = (
        (normalize(mixed_heads, sub_gain) * output_scale)
        .astype(jnp.bfloat16)
        .reshape(sequences * tokens_here, HEADS * HV)
    )
    projected = jnp.dot(
        normed,
        lax.all_gather(out_weight, "dp", axis=1, tiled=True),
        preferred_element_type=jnp.float32,
    )
    return projected.astype(jnp.bfloat16).reshape(sequences, tokens_here, D)


MESH = pl.DeviceIdType.MESH


def fits(sp, dp, rows_shape, weight_shape):
    if HEADS % sp or (HEADS // sp * HK) % 128 or dp % 2:
        return False
    return rows_shape[0] == 1 and rows_shape[1] % 128 == 0 and rows_shape[1] * sp <= 1024 and weight_shape[1] % 128 == 0


def kernel(
    sp, dp, q_ref, k_ref, v_ref, lam_in, qg_in, kg_in, sg_in, w_ref, out_ref,
    qb, kb, vb, kn, first, nsend, nbuf, wbuf,
    in_send, in_recv, back_send, back_recv, w_send, w_recv, p_send, p_recv, own_sem,
    lam_ref, qg_ref, kg_ref, sg_ref, small_sem,
):
    me, d = lax.axis_index("sp"), lax.axis_index("dp")
    partner = d + 1 - 2 * lax.rem(d, 2)
    chips = dp // 2
    rows = q_ref.shape[0]
    local = HEADS // sp
    width, vwidth = local * HK, local * HV
    depth, columns = w_ref.shape
    half = depth // 2
    square = chips == 4

    def fellow(c, device=d):
        if not square:
            return lax.rem(device + 2 * c, dp)
        core, chip = lax.rem(device, 2), device // 2
        x, y = lax.rem(chip, 2), chip // 2
        x = 1 - x if c % 2 else x
        y = 1 - y if c // 2 else y
        return (y * 2 + x) * 2 + core

    barrier = pltpu.get_barrier_semaphore()
    for o in range(1, sp):
        pl.semaphore_signal(barrier, inc=1, device_id=(lax.rem(me + o, sp), d), device_id_type=MESH)
    for c in range(1, chips):
        pl.semaphore_signal(barrier, inc=1, device_id=(me, fellow(c)), device_id_type=MESH)
    pl.semaphore_signal(barrier, inc=1, device_id=(me, partner), device_id_type=MESH)
    pl.semaphore_wait(barrier, sp - 1 + chips)

    def span(i):
        return pl.ds(pl.multiple_of(i * rows, rows), rows)

    def pieces(target, source):
        low = pl.ds(pl.multiple_of(target * width, 128), width)
        high = pl.ds(pl.multiple_of(HEADS * HK + target * width, 128), width)
        vals = pl.ds(pl.multiple_of(target * vwidth, 128), vwidth)
        there = span(source)
        return (
            (k_ref.at[:, low], kb.at[0, there, :]),
            (q_ref.at[:, low], qb.at[0, there, :]),
            (v_ref.at[:, vals], vb.at[there, :]),
            (k_ref.at[:, high], kb.at[1, there, :]),
            (q_ref.at[:, high], qb.at[1, there, :]),
        )

    def forward(o, t):
        target = lax.rem(me + o, sp)
        src, dst = pieces(target, me)[t]
        return pltpu.make_async_remote_copy(
            src_ref=src, dst_ref=dst, send_sem=in_send.at[o, t], recv_sem=in_recv.at[me, t],
            device_id=(target, d), device_id_type=MESH,
        )

    def mine(t):
        src, dst = pieces(me, me)[t]
        return pltpu.make_async_copy(src, dst, in_recv.at[me, t])

    def arrived(i, t):
        @pl.when(i == me)
        def _():
            mine(t).wait()

        @pl.when(i != me)
        def _():
            src, dst = pieces(me, i)[t]
            pltpu.make_async_remote_copy(
                src_ref=src, dst_ref=dst, send_sem=in_send.at[0, t], recv_sem=in_recv.at[i, t],
                device_id=(me, d), device_id_type=MESH,
            ).wait_recv()

    def rows_of(h):
        return pl.ds(h * half, half)

    def spread(c, h):
        source, over = d, c
        if square and c == 3:
            source, over = fellow(1 + h), 2 - h
        src = w_ref if source is d else wbuf.at[source]
        return pltpu.make_async_remote_copy(
            src_ref=src.at[rows_of(h)], dst_ref=wbuf.at[source, rows_of(h)], send_sem=w_send.at[c, h], recv_sem=w_recv.at[c, h],
            device_id=(me, fellow(over)), device_id_type=MESH,
        )

    def shard_of(device, c):
        if c == 0:
            return device
        return fellow(c, device) if square else lax.rem(device - 2 * c + dp, dp)

    def own_weights():
        return pltpu.make_async_copy(w_ref, wbuf.at[d], own_sem)

    def gained(c, h):
        at = shard_of(d, c)
        pltpu.make_async_remote_copy(
            src_ref=wbuf.at[at, rows_of(h)], dst_ref=wbuf.at[at, rows_of(h)], send_sem=w_send.at[c, h], recv_sem=w_recv.at[c, h],
            device_id=(me, partner), device_id_type=MESH,
        ).wait_recv()

    def pair(c):
        at = shard_of(d, c)
        return pltpu.make_async_remote_copy(
            src_ref=w_ref if c == 0 else wbuf.at[at], dst_ref=wbuf.at[at],
            send_sem=p_send.at[c], recv_sem=p_recv.at[c],
            device_id=(me, partner), device_id_type=MESH,
        )

    def back(i):
        return pltpu.make_async_remote_copy(
            src_ref=nsend.at[i], dst_ref=nbuf.at[me], send_sem=back_send.at[i], recv_sem=back_recv.at[me],
            device_id=(i, d), device_id_type=MESH,
        )

    small = [
        pltpu.make_async_copy(src, dst, small_sem.at[n])
        for n, (src, dst) in enumerate(((lam_in, lam_ref), (qg_in, qg_ref), (kg_in, kg_ref), (sg_in, sg_ref)))
    ]
    for t in range(5):
        mine(t).start()
        for o in range(1, sp):
            forward(o, t).start()
        if t == 0:
            for order in range(2):
                for c in range(1, chips):
                    if not (square and c == 3):
                        spread(c, (c + 1 + order) % 2).start()
            pair(0).start()
            own_weights().start()
            for copy in small:
                copy.start()
    if square:
        for h in range(2):
            gained(1 + h, h)
            spread(3, h).start()

    for copy in small:
        copy.wait()
    lane = lax.broadcasted_iota(jnp.int32, (width, width), 1) // HK
    ones = (lane == lax.broadcasted_iota(jnp.int32, (width, width), 0) // HK).astype(jnp.bfloat16)
    head_of = lax.broadcasted_iota(jnp.int32, (rows, width), 1) // HK
    visible = lax.broadcasted_iota(jnp.int32, (rows, rows), 1) <= lax.broadcasted_iota(jnp.int32, (rows, rows), 0)
    visible = jnp.concatenate([visible] * local, axis=0)
    query_gain = jnp.concatenate([qg_ref[...]] * local, axis=1)
    key_gain = jnp.concatenate([kg_ref[...]] * local, axis=1)
    sub_gain = sg_ref[...] * output_scale

    def normed_rows(block, gain):
        field = block.astype(jnp.float32)
        square = field * field
        upper = square.astype(jnp.bfloat16)
        lower = (square - upper.astype(jnp.float32)).astype(jnp.bfloat16)
        total = jnp.dot(upper, ones, preferred_element_type=jnp.float32)
        total += jnp.dot(lower, ones, preferred_element_type=jnp.float32)
        return (field * lax.rsqrt(total * (1.0 / HK) + epsilon) * gain).astype(jnp.bfloat16)

    def attend_block(m, i):
        base, keys = i * rows, (i + 1) * rows
        kn[m, base:keys, :] = normed_rows(kb[m, base:keys, :], key_gain)
        query = normed_rows(qb[m, base:keys, :], query_gain)
        zero = jnp.zeros_like(query)
        stacked = jnp.concatenate([jnp.where(head_of == h, query, zero) for h in range(local)], axis=0)
        scores = lax.dot_general(
            stacked, kn[m, :keys, :], (((1,), (1,)), ((), ())), preferred_element_type=jnp.float32
        ) * HK ** (-0.5)
        last = jnp.where(visible, scores[:, base:], -jnp.inf)
        scores = last if i == 0 else jnp.concatenate([scores[:, :base], last], axis=1)
        raised = jnp.exp(scores - jnp.max(scores, axis=1, keepdims=True))
        weights = (raised * (1.0 / jnp.sum(raised, axis=1, keepdims=True))).astype(jnp.bfloat16)
        return [
            jnp.dot(
                weights[h * rows : (h + 1) * rows], vb[:keys, h * HV : (h + 1) * HV],
                preferred_element_type=jnp.float32,
            ).astype(jnp.bfloat16)
            for h in range(local)
        ]

    for i in range(sp):
        for t in range(3):
            arrived(i, t)
        for h, part in enumerate(attend_block(0, i)):
            first[i * rows : (i + 1) * rows, h * HV : (h + 1) * HV] = part

    if square:
        for h in range(2):
            gained(1 + h, 1 - h)
            pair(1 + h).start()

    for i in range(sp):
        for t in range(3, 5):
            arrived(i, t)
        for h, part in enumerate(attend_block(1, i)):
            before = first[i * rows : (i + 1) * rows, h * HV : (h + 1) * HV].astype(jnp.float32)
            mixed = before - lam_ref[me * local + h] * part.astype(jnp.float32)
            mean = jnp.mean(mixed * mixed, axis=1, keepdims=True)
            nsend[i, :, h * HV : (h + 1) * HV] = (mixed * lax.rsqrt(mean + epsilon) * sub_gain).astype(jnp.bfloat16)

        @pl.when(i == me)
        def _():
            nbuf[i] = nsend[i]

        @pl.when(i != me)
        def _():
            back(i).start()

    for c in range(3 if square else 1, chips):
        for h in range(2):
            gained(c, h)
        pair(c).start()

    for i in range(sp):
        @pl.when(i != me)
        def _():
            pltpu.make_async_remote_copy(
                src_ref=nsend.at[i], dst_ref=nbuf.at[i], send_sem=back_send.at[i], recv_sem=back_recv.at[i],
                device_id=(i, d), device_id_type=MESH,
            ).wait_recv()

    normed = jnp.concatenate([nbuf[j] for j in range(sp)], axis=1)

    def project(shard, weight):
        out_ref[:, pl.ds(pl.multiple_of(shard * columns, 128), columns)] = jnp.dot(
            normed, weight, preferred_element_type=jnp.float32
        ).astype(jnp.bfloat16)

    own_weights().wait()
    for c in range(chips):
        project(shard_of(d, c), wbuf[shard_of(d, c)])
    for c in range(chips):
        at = shard_of(partner, c)
        pltpu.make_async_remote_copy(
            src_ref=wbuf.at[at], dst_ref=wbuf.at[at], send_sem=p_send.at[c], recv_sem=p_recv.at[c],
            device_id=(me, partner), device_id_type=MESH,
        ).wait_recv()
        project(at, wbuf[at])

    for o in range(1, sp):
        for t in range(5):
            forward(o, t).wait_send()
    for c in range(chips):
        pair(c).wait_send()
        if c:
            for h in range(2):
                spread(c, h).wait_send()
    for i in range(sp):
        @pl.when(i != me)
        def _():
            back(i).wait_send()


def fused(sp, dp, query_rows, key_rows, value_rows, lambdas, query_gain, key_gain, sub_gain, out_weight):
    rows = query_rows.shape[1]
    length = rows * sp
    local = HEADS // sp
    width, vwidth = local * HK, local * HV
    depth, columns = out_weight.shape
    vmem = pl.BlockSpec(memory_space=pltpu.VMEM)
    hbm = pl.BlockSpec(memory_space=pl.ANY)
    dma = pltpu.SemaphoreType.DMA
    out = pl.pallas_call(
        functools.partial(kernel, sp, dp),
        out_shape=pltpu.VMEM((rows, columns * dp), jnp.bfloat16),
        in_specs=[hbm] * 8,
        out_specs=vmem,
        scratch_shapes=[
            pltpu.VMEM((2, length, width), jnp.bfloat16),
            pltpu.VMEM((2, length, width), jnp.bfloat16),
            pltpu.VMEM((length, vwidth), jnp.bfloat16),
            pltpu.VMEM((2, length, width), jnp.bfloat16),
            pltpu.VMEM((length, vwidth), jnp.bfloat16),
            pltpu.VMEM((sp, rows, vwidth), jnp.bfloat16),
            pltpu.VMEM((sp, rows, vwidth), jnp.bfloat16),
            pltpu.VMEM((dp, depth, columns), jnp.bfloat16),
            dma((sp, 5)), dma((sp, 5)), dma((sp,)), dma((sp,)),
            dma((dp // 2, 2)), dma((dp // 2, 2)), dma((dp // 2,)), dma((dp // 2,)), dma,
            pltpu.SMEM(lambdas.shape, jnp.float32),
            pltpu.VMEM((1, HK), jnp.float32), pltpu.VMEM((1, HK), jnp.float32), pltpu.VMEM((1, HV), jnp.float32),
            dma((4,)),
        ],
        compiler_params=pltpu.CompilerParams(collective_id=0, has_side_effects=True),
    )(
        query_rows[0], key_rows[0], value_rows[0], lambdas,
        query_gain[None], key_gain[None], sub_gain[None], out_weight,
    )
    return out[None]


def solution(mesh):
    in_specs = (
        P("dp", "sp", None),
        P("dp", "sp", None),
        P("dp", "sp", None),
        P(),
        P(),
        P(),
        P(),
        P(None, "dp"),
    )
    out_specs = P("dp", "sp", None)
    sp, dp = mesh.shape["sp"], mesh.shape["dp"]

    def step(*operands):
        if fits(sp, dp, operands[0].shape, operands[7].shape):
            return fused(sp, dp, *operands)
        return body(*operands)

    return jax.shard_map(step, mesh=mesh, in_specs=in_specs, out_specs=out_specs, check_vma=False)
```

```python
import functools

import jax
import jax.numpy as jnp
from jax import lax
from jax.experimental import pallas as pl
from jax.experimental.pallas import tpu as pltpu
from jax.sharding import PartitionSpec as P

D = 2048
HEADS = 8
HK = 64
HV = 128


epsilon = 1e-06
output_scale = 0.8


def normalize(field, scaling):
    return field * lax.rsqrt(jnp.mean(field * field, axis=-1, keepdims=True) + epsilon) * scaling


def attend(arrived, length):
    block_rows = max(min(512, length), length // 16)
    results = []
    for number in range(length // block_rows):
        first_row = number * block_rows
        last_row = first_row + block_rows
        query_block = arrived[first_row:last_row, :, :HK]
        key_block = arrived[:last_row, :, HK : 2 * HK]
        value_block = arrived[:last_row, :, 2 * HK :]
        scores = jnp.einsum(
            "qgd,kgd->gqk", query_block, key_block, preferred_element_type=jnp.float32
        ) * HK ** (-0.5)
        visible = jnp.arange(last_row)[None, :] <= (first_row + jnp.arange(block_rows))[:, None]
        scores = jnp.where(visible[None], scores, -jnp.inf)
        weights = jax.nn.softmax(scores, axis=-1).astype(jnp.bfloat16)
        results.append(
            jnp.einsum(
                "gqk,kgd->qgd", weights, value_block, preferred_element_type=jnp.float32
            ).astype(jnp.bfloat16)
        )
    return jnp.concatenate(results, axis=0)


def body(query_rows, key_rows, value_rows, lambdas, query_gain, key_gain, sub_gain, out_weight):
    sequences = query_rows.shape[0]
    tokens_here = query_rows.shape[1]
    groups = 2 * HEADS
    query_norm = normalize(
        query_rows.reshape(sequences, tokens_here, groups, HK).astype(jnp.float32), query_gain
    ).astype(jnp.bfloat16)
    key_norm = normalize(
        key_rows.reshape(sequences, tokens_here, groups, HK).astype(jnp.float32), key_gain
    ).astype(jnp.bfloat16)
    value_heads = value_rows.reshape(sequences, tokens_here, HEADS, HV)
    packet = jnp.concatenate(
        [query_norm, key_norm, jnp.concatenate([value_heads, value_heads], axis=2)], axis=3
    )
    arrived = lax.all_to_all(packet, "sp", split_axis=2, concat_axis=1, tiled=True)
    length = arrived.shape[1]
    map_outputs = attend(arrived[0], length)[None]
    returned = lax.all_to_all(map_outputs, "sp", split_axis=1, concat_axis=2, tiled=True)
    returned_float = returned.astype(jnp.float32)
    mixed_heads = returned_float[:, :, :HEADS] - lambdas[:, None] * returned_float[:, :, HEADS:]
    normed = (
        (normalize(mixed_heads, sub_gain) * output_scale)
        .astype(jnp.bfloat16)
        .reshape(sequences * tokens_here, HEADS * HV)
    )
    projected = jnp.dot(
        normed,
        lax.all_gather(out_weight, "dp", axis=1, tiled=True),
        preferred_element_type=jnp.float32,
    )
    return projected.astype(jnp.bfloat16).reshape(sequences, tokens_here, D)


MESH = pl.DeviceIdType.MESH


def fits(sp, dp, rows_shape, weight_shape):
    if sp != 4 or HEADS % sp or (HEADS // sp * HK) % 128 or dp % 2:
        return False
    return rows_shape[0] == 1 and rows_shape[1] % 128 == 0 and rows_shape[1] * sp <= 1024 and weight_shape[1] % 128 == 0


def kernel(
    sp, dp, q_ref, k_ref, v_ref, lam_in, qg_in, kg_in, sg_in, w_ref, out_ref,
    qb, kb, vb, kn, qx, kx, vx, knx, nsend, nbuf, wbuf,
    local_sem, in_send, in_recv, back_send, back_recv, w_send, w_recv, p_send, p_recv, own_sem,
    lam_ref, qg_ref, kg_ref, sg_ref, small_sem,
):
    me, d = lax.axis_index("sp"), lax.axis_index("dp")
    partner = d + 1 - 2 * lax.rem(d, 2)
    chips = dp // 2
    rows = q_ref.shape[0]
    local = HEADS // sp
    width, vwidth = local * HK, local * HV
    depth, columns = w_ref.shape
    half = depth // 2
    square = chips == 4

    def fellow(c, device=d):
        if not square:
            return lax.rem(device + 2 * c, dp)
        core, chip = lax.rem(device, 2), device // 2
        x, y = lax.rem(chip, 2), chip // 2
        x = 1 - x if c % 2 else x
        y = 1 - y if c // 2 else y
        return (y * 2 + x) * 2 + core

    barrier = pltpu.get_barrier_semaphore()
    for o in range(1, sp):
        pl.semaphore_signal(barrier, inc=1, device_id=(lax.rem(me + o, sp), d), device_id_type=MESH)
    for c in range(1, chips):
        pl.semaphore_signal(barrier, inc=1, device_id=(me, fellow(c)), device_id_type=MESH)
    pl.semaphore_signal(barrier, inc=1, device_id=(me, partner), device_id_type=MESH)
    pl.semaphore_wait(barrier, sp - 1 + chips)

    half_sp = sp // 2
    lows, highs = range(half_sp), range(half_sp, sp)

    def at(i):
        return pl.ds(i * rows, rows)

    def cols(pair_, m=0, count=1):
        return pl.ds(m * HEADS * HK + pair_ * width, count * width)

    def vcols(pair_, count=1):
        return pl.ds(pair_ * vwidth, count * vwidth)

    plan = {}
    for z in range(sp):
        for o in range(sp):
            for m in range(2):
                if o != z and (o in lows or z in highs):
                    plan[z, o, "q", m] = q_ref.at[:, cols(o, m)], qb.at[m, at(z), :]
                if o != z and (o in lows or z != 0):
                    plan[z, o, "k", m] = k_ref.at[:, cols(o, m)], kb.at[m, at(z), :]
            if o != z and (o in lows or z != 0):
                plan[z, o, "v", 0] = v_ref.at[:, vcols(o)], vb.at[at(z), :]
    for m in range(2):
        plan[0, 1, "kx", m] = k_ref.at[:, cols(half_sp, m, half_sp)], kx.at[m, at(0), :]
    plan[0, 1, "vx", 0] = v_ref.at[:, vcols(half_sp, half_sp)], vx.at[at(0), :]
    for o in highs:
        for m in range(2):
            plan[1, o, "rk", m] = kx.at[m, at(0), cols(o - half_sp)], kb.at[m, at(0), :]
        plan[1, o, "rv", 0] = vx.at[at(0), vcols(o - half_sp)], vb.at[at(0), :]
    number = {key: n for n, key in enumerate(plan)}

    def move(*key):
        src, dst = plan[key]
        n = number[key]
        return pltpu.make_async_remote_copy(
            src_ref=src, dst_ref=dst, send_sem=in_send.at[n], recv_sem=in_recv.at[n],
            device_id=(key[1], d), device_id_type=MESH,
        )

    def rows_in(z):
        copies = []
        for m in range(2):
            copies.append((k_ref.at[:, cols(z, m)], kb.at[m, at(z), :]))
            copies.append((q_ref.at[:, cols(z, m)], qb.at[m, at(z), :]))
            if z in lows:
                copies.append((k_ref.at[:, cols(half_sp, m, half_sp)], kx.at[m, at(z), :]))
                copies.append((q_ref.at[:, cols(half_sp, m, half_sp)], qx.at[m]))
        copies.append((v_ref.at[:, vcols(z)], vb.at[at(z), :]))
        if z in lows:
            copies.append((v_ref.at[:, vcols(half_sp, half_sp)], vx.at[at(z), :]))
        return [pltpu.make_async_copy(src, dst, local_sem.at[n]) for n, (src, dst) in enumerate(copies)]

    five = (("k", 0), ("q", 0), ("v", 0), ("k", 1), ("q", 1))
    three = (("k", 0), ("v", 0), ("k", 1))

    def outgoing(z):
        if z == 0:
            return [(0, 1, "kx", 0), (0, 1, "vx", 0), (0, 1, "kx", 1)] + [(0, 1) + f for f in five]
        if z == 1:
            return [(1, o) + f for f in three for o in highs] + [(1, 0) + f for f in five]
        if z == 2:
            return [(2, 0) + f for f in five] + [(2, 1) + f for f in five] + [(2, 3) + f for f in five]
        return [(3, 0) + f for f in five] + [(3, 2) + f for f in five] + [(3, 1) + f for f in five]

    relays = (("kx", "rk", 0), ("vx", "rv", 0), ("kx", "rk", 1))

    def rows_of(h):
        return pl.ds(h * half, half)

    def spread(c, h):
        source, over = d, c
        if square and c == 3:
            source, over = fellow(1 + h), 2 - h
        src = w_ref if source is d else wbuf.at[source]
        return pltpu.make_async_remote_copy(
            src_ref=src.at[rows_of(h)], dst_ref=wbuf.at[source, rows_of(h)], send_sem=w_send.at[c, h], recv_sem=w_recv.at[c, h],
            device_id=(me, fellow(over)), device_id_type=MESH,
        )

    def shard_of(device, c):
        if c == 0:
            return device
        return fellow(c, device) if square else lax.rem(device - 2 * c + dp, dp)

    def own_weights():
        return pltpu.make_async_copy(w_ref, wbuf.at[d], own_sem)

    def gained(c, h):
        at = shard_of(d, c)
        pltpu.make_async_remote_copy(
            src_ref=wbuf.at[at, rows_of(h)], dst_ref=wbuf.at[at, rows_of(h)], send_sem=w_send.at[c, h], recv_sem=w_recv.at[c, h],
            device_id=(me, partner), device_id_type=MESH,
        ).wait_recv()

    def pair(c):
        at = shard_of(d, c)
        return pltpu.make_async_remote_copy(
            src_ref=w_ref if c == 0 else wbuf.at[at], dst_ref=wbuf.at[at],
            send_sem=p_send.at[c], recv_sem=p_recv.at[c],
            device_id=(me, partner), device_id_type=MESH,
        )

    def back(z, i):
        return pltpu.make_async_remote_copy(
            src_ref=nsend.at[i], dst_ref=nbuf.at[z], send_sem=back_send.at[i], recv_sem=back_recv.at[z],
            device_id=(i, d), device_id_type=MESH,
        )

    small = [
        pltpu.make_async_copy(src, dst, small_sem.at[n])
        for n, (src, dst) in enumerate(((lam_in, lam_ref), (qg_in, qg_ref), (kg_in, kg_ref), (sg_in, sg_ref)))
    ]
    for z in range(sp):
        @pl.when(me == z)
        def _(z=z):
            for key in outgoing(z):
                move(*key).start()

    for order in range(2):
        for c in range(1, chips):
            if not (square and c == 3):
                spread(c, (c + 1 + order) % 2).start()
    pair(0).start()
    for z in range(sp):
        @pl.when(me == z)
        def _(z=z):
            for copy in rows_in(z):
                copy.start()
    own_weights().start()
    for copy in small:
        copy.start()
    for copy in small:
        copy.wait()

    def weights_first():
        if square:
            for h in range(2):
                gained(1 + h, h)
                spread(3, h).start()

    def weights_next():
        if square:
            for h in range(2):
                gained(1 + h, 1 - h)
                pair(1 + h).start()

    def weights_last():
        for c in range(3 if square else 1, chips):
            for h in range(2):
                gained(c, h)
            pair(c).start()

    lane = lax.broadcasted_iota(jnp.int32, (width, width), 1) // HK
    ones = (lane == lax.broadcasted_iota(jnp.int32, (width, width), 0) // HK).astype(jnp.bfloat16)
    head_of = lax.broadcasted_iota(jnp.int32, (rows, width), 1) // HK
    visible = lax.broadcasted_iota(jnp.int32, (rows, rows), 1) <= lax.broadcasted_iota(jnp.int32, (rows, rows), 0)
    visible = jnp.concatenate([visible] * local, axis=0)
    query_gain = jnp.concatenate([qg_ref[...]] * local, axis=1)
    key_gain = jnp.concatenate([kg_ref[...]] * local, axis=1)
    sub_gain = sg_ref[...] * output_scale

    def normed_rows(block, gain):
        field = block.astype(jnp.float32)
        square = field * field
        upper = square.astype(jnp.bfloat16)
        lower = (square - upper.astype(jnp.float32)).astype(jnp.bfloat16)
        total = jnp.dot(upper, ones, preferred_element_type=jnp.float32)
        total += jnp.dot(lower, ones, preferred_element_type=jnp.float32)
        return (field * lax.rsqrt(total * (1.0 / HK) + epsilon) * gain).astype(jnp.bfloat16)

    def attend(query, keys, vals, before):
        query = normed_rows(query, query_gain)
        zero = jnp.zeros_like(query)
        stacked = jnp.concatenate([jnp.where(head_of == h, query, zero) for h in range(local)], axis=0)
        scores = lax.dot_general(
            stacked, keys, (((1,), (1,)), ((), ())), preferred_element_type=jnp.float32
        ) * HK ** (-0.5)
        last = jnp.where(visible, scores[:, before:], -jnp.inf)
        scores = last if before == 0 else jnp.concatenate([scores[:, :before], last], axis=1)
        raised = jnp.exp(scores - jnp.max(scores, axis=1, keepdims=True))
        weights = (raised * (1.0 / jnp.sum(raised, axis=1, keepdims=True))).astype(jnp.bfloat16)
        return [
            jnp.dot(
                weights[h * rows : (h + 1) * rows], vals[:, h * HV : (h + 1) * HV],
                preferred_element_type=jnp.float32,
            ).astype(jnp.bfloat16)
            for h in range(local)
        ]

    def mix(pair_, maps):
        parts = []
        for h in range(local):
            mixed = maps[0][h].astype(jnp.float32) - lam_ref[pair_ * local + h] * maps[1][h].astype(jnp.float32)
            mean = jnp.mean(mixed * mixed, axis=1, keepdims=True)
            parts.append((mixed * lax.rsqrt(mean + epsilon) * sub_gain).astype(jnp.bfloat16))
        return jnp.concatenate(parts, axis=1)

    def new_keys(m, i):
        kn[m, i * rows : (i + 1) * rows, :] = normed_rows(kb[m, i * rows : (i + 1) * rows, :], key_gain)

    def pair_map(m, i):
        keys = (i + 1) * rows
        return attend(qb[m, i * rows : keys, :], kn[m, :keys, :], vb[:keys, :], i * rows)

    def near(z):
        keys = (z + 1) * rows
        for p in range(half_sp):
            maps = []
            for m in range(2):
                for i in range(z + 1):
                    knx[m, i * rows : (i + 1) * rows, :] = normed_rows(
                        kx[m, i * rows : (i + 1) * rows, p * width : (p + 1) * width], key_gain
                    )
                maps.append(attend(
                    qx[m, :, p * width : (p + 1) * width], knx[m, :keys, :],
                    vx[:keys, p * vwidth : (p + 1) * vwidth], z * rows,
                ))
            nbuf[half_sp + p] = mix(half_sp + p, maps)

    def give(z, i, maps):
        if i == z:
            nbuf[z] = mix(z, maps)
        else:
            nsend[i] = mix(z, maps)
            back(z, i).start()

    def below(z):
        for copy in rows_in(z):
            copy.wait()
        if z == 1:
            for held, sent, m in relays:
                move(0, 1, held, m).wait_recv()
                for o in highs:
                    move(1, o, sent, m).start()
        near(z)
        weights_first()
        for i in range(sp):
            maps = []
            for m in range(2):
                if i != z:
                    for f in five[3 * m : 3 + 2 * m]:
                        move(i, z, *f).wait_recv()
                new_keys(m, i)
                maps.append(pair_map(m, i))
            give(z, i, maps)
            if i == half_sp:
                weights_next()

    def above(z):
        for copy in rows_in(z):
            copy.wait()
        weights_first()
        weights_next()
        other = half_sp + sp - 1 - z
        both = {i: [] for i in highs}
        for m in range(2):
            for f in five[3 * m : 3 + 2 * m]:
                move(other, z, *f).wait_recv()
                if f[0] != "q":
                    move(1, z, *f).wait_recv()
                    move(0 + 1, z, "r" + f[0], f[1]).wait_recv()
            for i in range(sp):
                new_keys(m, i)
            for i in (other, z):
                both[i].append(pair_map(m, i))
        for i in (other, z):
            give(z, i, both[i])

    for z in range(sp):
        @pl.when(me == z)
        def _(z=z):
            below(z) if z in lows else above(z)

    weights_last()
    for z in range(sp):
        @pl.when(me == z)
        def _(z=z):
            for o in range(sp):
                if o != z and (o in lows or z in highs):
                    back(o, z).wait_recv()

    normed = jnp.concatenate([nbuf[j] for j in range(sp)], axis=1)

    def project(shard, weight):
        out_ref[:, pl.ds(pl.multiple_of(shard * columns, 128), columns)] = jnp.dot(
            normed, weight, preferred_element_type=jnp.float32
        ).astype(jnp.bfloat16)

    own_weights().wait()
    for c in range(chips):
        project(shard_of(d, c), wbuf[shard_of(d, c)])
    for c in range(chips):
        at = shard_of(partner, c)
        pltpu.make_async_remote_copy(
            src_ref=wbuf.at[at], dst_ref=wbuf.at[at], send_sem=p_send.at[c], recv_sem=p_recv.at[c],
            device_id=(me, partner), device_id_type=MESH,
        ).wait_recv()
        project(at, wbuf[at])

    for z in range(sp):
        @pl.when(me == z)
        def _(z=z):
            for key in outgoing(z):
                move(*key).wait_send()
            if z == 1:
                for _, sent, m in relays:
                    for o in highs:
                        move(1, o, sent, m).wait_send()
            for i in range(sp):
                if i != z and (z in lows or i in highs):
                    back(z, i).wait_send()
    for c in range(chips):
        pair(c).wait_send()
        if c:
            for h in range(2):
                spread(c, h).wait_send()


def fused(sp, dp, query_rows, key_rows, value_rows, lambdas, query_gain, key_gain, sub_gain, out_weight):
    rows = query_rows.shape[1]
    length = rows * sp
    local = HEADS // sp
    width, vwidth = local * HK, local * HV
    depth, columns = out_weight.shape
    vmem = pl.BlockSpec(memory_space=pltpu.VMEM)
    hbm = pl.BlockSpec(memory_space=pl.ANY)
    dma = pltpu.SemaphoreType.DMA
    out = pl.pallas_call(
        functools.partial(kernel, sp, dp),
        out_shape=pltpu.VMEM((rows, columns * dp), jnp.bfloat16),
        in_specs=[hbm] * 8,
        out_specs=vmem,
        scratch_shapes=[
            pltpu.VMEM((2, length, width), jnp.bfloat16),
            pltpu.VMEM((2, length, width), jnp.bfloat16),
            pltpu.VMEM((length, vwidth), jnp.bfloat16),
            pltpu.VMEM((2, length, width), jnp.bfloat16),
            pltpu.VMEM((2, rows, sp // 2 * width), jnp.bfloat16),
            pltpu.VMEM((2, sp // 2 * rows, sp // 2 * width), jnp.bfloat16),
            pltpu.VMEM((sp // 2 * rows, sp // 2 * vwidth), jnp.bfloat16),
            pltpu.VMEM((2, sp // 2 * rows, width), jnp.bfloat16),
            pltpu.VMEM((sp, rows, vwidth), jnp.bfloat16),
            pltpu.VMEM((sp, rows, vwidth), jnp.bfloat16),
            pltpu.VMEM((dp, depth, columns), jnp.bfloat16),
            dma((10,)), dma((5 * sp * sp,)), dma((5 * sp * sp,)), dma((sp,)), dma((sp,)),
            dma((dp // 2, 2)), dma((dp // 2, 2)), dma((dp // 2,)), dma((dp // 2,)), dma,
            pltpu.SMEM(lambdas.shape, jnp.float32),
            pltpu.VMEM((1, HK), jnp.float32), pltpu.VMEM((1, HK), jnp.float32), pltpu.VMEM((1, HV), jnp.float32),
            dma((4,)),
        ],
        compiler_params=pltpu.CompilerParams(collective_id=0, has_side_effects=True),
    )(
        query_rows[0], key_rows[0], value_rows[0], lambdas,
        query_gain[None], key_gain[None], sub_gain[None], out_weight,
    )
    return out[None]


def solution(mesh):
    in_specs = (
        P("dp", "sp", None),
        P("dp", "sp", None),
        P("dp", "sp", None),
        P(),
        P(),
        P(),
        P(),
        P(None, "dp"),
    )
    out_specs = P("dp", "sp", None)
    sp, dp = mesh.shape["sp"], mesh.shape["dp"]

    def step(*operands):
        if fits(sp, dp, operands[0].shape, operands[7].shape):
            return fused(sp, dp, *operands)
        return body(*operands)

    return jax.shard_map(step, mesh=mesh, in_specs=in_specs, out_specs=out_specs, check_vma=False)
```

```python
import functools

import jax
import jax.numpy as jnp
from jax import lax
from jax.experimental import pallas as pl
from jax.experimental.pallas import tpu as pltpu
from jax.sharding import PartitionSpec as P

D = 2048
HEADS = 8
HK = 64
HV = 128


epsilon = 1e-06
output_scale = 0.8


def normalize(field, scaling):
    return field * lax.rsqrt(jnp.mean(field * field, axis=-1, keepdims=True) + epsilon) * scaling


def attend(arrived, length):
    block_rows = max(min(512, length), length // 16)
    results = []
    for number in range(length // block_rows):
        first_row = number * block_rows
        last_row = first_row + block_rows
        query_block = arrived[first_row:last_row, :, :HK]
        key_block = arrived[:last_row, :, HK : 2 * HK]
        value_block = arrived[:last_row, :, 2 * HK :]
        scores = jnp.einsum(
            "qgd,kgd->gqk", query_block, key_block, preferred_element_type=jnp.float32
        ) * HK ** (-0.5)
        visible = jnp.arange(last_row)[None, :] <= (first_row + jnp.arange(block_rows))[:, None]
        scores = jnp.where(visible[None], scores, -jnp.inf)
        weights = jax.nn.softmax(scores, axis=-1).astype(jnp.bfloat16)
        results.append(
            jnp.einsum(
                "gqk,kgd->qgd", weights, value_block, preferred_element_type=jnp.float32
            ).astype(jnp.bfloat16)
        )
    return jnp.concatenate(results, axis=0)


def body(query_rows, key_rows, value_rows, lambdas, query_gain, key_gain, sub_gain, out_weight):
    sequences = query_rows.shape[0]
    tokens_here = query_rows.shape[1]
    groups = 2 * HEADS
    query_norm = normalize(
        query_rows.reshape(sequences, tokens_here, groups, HK).astype(jnp.float32), query_gain
    ).astype(jnp.bfloat16)
    key_norm = normalize(
        key_rows.reshape(sequences, tokens_here, groups, HK).astype(jnp.float32), key_gain
    ).astype(jnp.bfloat16)
    value_heads = value_rows.reshape(sequences, tokens_here, HEADS, HV)
    packet = jnp.concatenate(
        [query_norm, key_norm, jnp.concatenate([value_heads, value_heads], axis=2)], axis=3
    )
    arrived = lax.all_to_all(packet, "sp", split_axis=2, concat_axis=1, tiled=True)
    length = arrived.shape[1]
    map_outputs = attend(arrived[0], length)[None]
    returned = lax.all_to_all(map_outputs, "sp", split_axis=1, concat_axis=2, tiled=True)
    returned_float = returned.astype(jnp.float32)
    mixed_heads = returned_float[:, :, :HEADS] - lambdas[:, None] * returned_float[:, :, HEADS:]
    normed = (
        (normalize(mixed_heads, sub_gain) * output_scale)
        .astype(jnp.bfloat16)
        .reshape(sequences * tokens_here, HEADS * HV)
    )
    projected = jnp.dot(
        normed,
        lax.all_gather(out_weight, "dp", axis=1, tiled=True),
        preferred_element_type=jnp.float32,
    )
    return projected.astype(jnp.bfloat16).reshape(sequences, tokens_here, D)


MESH = pl.DeviceIdType.MESH


def fits(sp, dp, rows_shape, weight_shape):
    if sp != 4 or HEADS % sp or (HEADS // sp * HK) % 128 or dp % 2:
        return False
    return rows_shape[0] == 1 and rows_shape[1] % 128 == 0 and rows_shape[1] * sp <= 1024 and weight_shape[1] % 128 == 0


def kernel(
    sp, dp, q_ref, k_ref, v_ref, lam_in, qg_in, kg_in, sg_in, w_ref, out_ref,
    qb, kb, vb, kn, qx, kx, vx, knx, nsend, nbuf, wbuf,
    local_sem, in_send, in_recv, back_send, back_recv, w_send, w_recv, p_send, p_recv, own_sem,
    lam_ref, qg_ref, kg_ref, sg_ref, small_sem, acc,
):
    me, d = lax.axis_index("sp"), lax.axis_index("dp")
    partner = d + 1 - 2 * lax.rem(d, 2)
    chips = dp // 2
    rows = q_ref.shape[0]
    local = HEADS // sp
    width, vwidth = local * HK, local * HV
    depth, columns = w_ref.shape
    half = depth // 2
    square = chips == 4

    def fellow(c, device=d):
        if not square:
            return lax.rem(device + 2 * c, dp)
        core, chip = lax.rem(device, 2), device // 2
        x, y = lax.rem(chip, 2), chip // 2
        x = 1 - x if c % 2 else x
        y = 1 - y if c // 2 else y
        return (y * 2 + x) * 2 + core

    barrier = pltpu.get_barrier_semaphore()
    for o in range(1, sp):
        pl.semaphore_signal(barrier, inc=1, device_id=(lax.rem(me + o, sp), d), device_id_type=MESH)
    for c in range(1, chips):
        pl.semaphore_signal(barrier, inc=1, device_id=(me, fellow(c)), device_id_type=MESH)
    pl.semaphore_signal(barrier, inc=1, device_id=(me, partner), device_id_type=MESH)

    half_sp = sp // 2
    lows, highs = range(half_sp), range(half_sp, sp)

    def at(i):
        return pl.ds(i * rows, rows)

    def cols(pair_, m=0, count=1):
        return pl.ds(m * HEADS * HK + pair_ * width, count * width)

    def vcols(pair_, count=1):
        return pl.ds(pair_ * vwidth, count * vwidth)

    plan = {}
    for z in range(sp):
        for o in range(sp):
            for m in range(2):
                if o != z and (o in lows or z in highs):
                    plan[z, o, "q", m] = q_ref.at[:, cols(o, m)], qb.at[m, at(z), :]
                if o != z and (o in lows or z != 0):
                    plan[z, o, "k", m] = k_ref.at[:, cols(o, m)], kb.at[m, at(z), :]
            if o != z and (o in lows or z != 0):
                plan[z, o, "v", 0] = v_ref.at[:, vcols(o)], vb.at[at(z), :]
    for m in range(2):
        plan[0, 1, "kx", m] = k_ref.at[:, cols(half_sp, m, half_sp)], kx.at[m, at(0), :]
    plan[0, 1, "vx", 0] = v_ref.at[:, vcols(half_sp, half_sp)], vx.at[at(0), :]
    for o in highs:
        for m in range(2):
            plan[1, o, "rk", m] = kx.at[m, at(0), cols(o - half_sp)], kb.at[m, at(0), :]
        plan[1, o, "rv", 0] = vx.at[at(0), vcols(o - half_sp)], vb.at[at(0), :]
    number = {key: n for n, key in enumerate(plan)}

    def move(*key):
        src, dst = plan[key]
        n = number[key]
        return pltpu.make_async_remote_copy(
            src_ref=src, dst_ref=dst, send_sem=in_send.at[n], recv_sem=in_recv.at[n],
            device_id=(key[1], d), device_id_type=MESH,
        )

    def rows_in(z):
        copies = []
        for m in range(2):
            copies.append((k_ref.at[:, cols(z, m)], kb.at[m, at(z), :]))
            copies.append((q_ref.at[:, cols(z, m)], qb.at[m, at(z), :]))
            if z in lows:
                copies.append((k_ref.at[:, cols(half_sp, m, half_sp)], kx.at[m, at(z), :]))
                copies.append((q_ref.at[:, cols(half_sp, m, half_sp)], qx.at[m]))
        copies.append((v_ref.at[:, vcols(z)], vb.at[at(z), :]))
        if z in lows:
            copies.append((v_ref.at[:, vcols(half_sp, half_sp)], vx.at[at(z), :]))
        return [pltpu.make_async_copy(src, dst, local_sem.at[n]) for n, (src, dst) in enumerate(copies)]

    five = (("k", 0), ("q", 0), ("v", 0), ("k", 1), ("q", 1))
    three = (("k", 0), ("v", 0), ("k", 1))

    def outgoing(z):
        if z == 0:
            return [(0, 1, "kx", 0), (0, 1, "vx", 0), (0, 1, "kx", 1)] + [(0, 1) + f for f in five]
        if z == 1:
            return [(1, o) + f for f in three for o in highs] + [(1, 0) + f for f in five]
        if z == 2:
            return [(2, 0) + f for f in five] + [(2, 1) + f for f in five] + [(2, 3) + f for f in five]
        return [(3, 0) + f for f in five] + [(3, 1) + f for f in five] + [(3, 2) + f for f in five]

    relays = (("kx", "rk", 0), ("vx", "rv", 0), ("kx", "rk", 1))

    def rows_of(h):
        return pl.ds(h * half, half)

    def spread(c, h):
        source, over = d, c
        if square and c == 3:
            source, over = fellow(1 + h), 2 - h
        src = w_ref if source is d else wbuf.at[source]
        return pltpu.make_async_remote_copy(
            src_ref=src.at[rows_of(h)], dst_ref=wbuf.at[source, rows_of(h)], send_sem=w_send.at[c, h], recv_sem=w_recv.at[c, h],
            device_id=(me, fellow(over)), device_id_type=MESH,
        )

    def shard_of(device, c):
        if c == 0:
            return device
        return fellow(c, device) if square else lax.rem(device - 2 * c + dp, dp)

    def own_weights():
        return pltpu.make_async_copy(w_ref, wbuf.at[d], own_sem)

    def gained(c, h):
        at = shard_of(d, c)
        pltpu.make_async_remote_copy(
            src_ref=wbuf.at[at, rows_of(h)], dst_ref=wbuf.at[at, rows_of(h)], send_sem=w_send.at[c, h], recv_sem=w_recv.at[c, h],
            device_id=(me, partner), device_id_type=MESH,
        ).wait_recv()

    def pair(c):
        at = shard_of(d, c)
        return pltpu.make_async_remote_copy(
            src_ref=w_ref if c == 0 else wbuf.at[at], dst_ref=wbuf.at[at],
            send_sem=p_send.at[c], recv_sem=p_recv.at[c],
            device_id=(me, partner), device_id_type=MESH,
        )

    def back(z, i):
        return pltpu.make_async_remote_copy(
            src_ref=nsend.at[i], dst_ref=nbuf.at[z], send_sem=back_send.at[i], recv_sem=back_recv.at[z],
            device_id=(i, d), device_id_type=MESH,
        )

    small = [
        pltpu.make_async_copy(src, dst, small_sem.at[n])
        for n, (src, dst) in enumerate(((lam_in, lam_ref), (qg_in, qg_ref), (kg_in, kg_ref), (sg_in, sg_ref)))
    ]
    for z in range(sp):
        @pl.when(me == z)
        def _(z=z):
            for copy in rows_in(z):
                copy.start()
    own_weights().start()
    for copy in small:
        copy.start()
    pl.semaphore_wait(barrier, sp - 1 + chips)

    for z in range(sp):
        @pl.when(me == z)
        def _(z=z):
            for key in outgoing(z):
                move(*key).start()

    for order in range(2):
        for c in range(1, chips):
            if not (square and c == 3):
                spread(c, (c + 1 + order) % 2).start()
    pair(0).start()
    for copy in small:
        copy.wait()

    def weights_first():
        if square:
            for h in range(2):
                gained(1 + h, h)
                spread(3, h).start()

    def weights_next():
        if square:
            for h in range(2):
                gained(1 + h, 1 - h)
                pair(1 + h).start()

    def weights_last():
        for c in range(3 if square else 1, chips):
            for h in range(2):
                gained(c, h)
            pair(c).start()

    lane = lax.broadcasted_iota(jnp.int32, (width, width), 1) // HK
    ones = (lane == lax.broadcasted_iota(jnp.int32, (width, width), 0) // HK).astype(jnp.bfloat16)
    head_of = lax.broadcasted_iota(jnp.int32, (rows, width), 1) // HK
    visible = lax.broadcasted_iota(jnp.int32, (rows, rows), 1) <= lax.broadcasted_iota(jnp.int32, (rows, rows), 0)
    visible = jnp.concatenate([visible] * local, axis=0)
    query_gain = jnp.concatenate([qg_ref[...]] * local, axis=1)
    key_gain = jnp.concatenate([kg_ref[...]] * local, axis=1)
    sub_gain = sg_ref[...] * output_scale

    def normed_rows(block, gain):
        field = block.astype(jnp.float32)
        square = field * field
        upper = square.astype(jnp.bfloat16)
        lower = (square - upper.astype(jnp.float32)).astype(jnp.bfloat16)
        total = jnp.dot(upper, ones, preferred_element_type=jnp.float32)
        total += jnp.dot(lower, ones, preferred_element_type=jnp.float32)
        return (field * lax.rsqrt(total * (1.0 / HK) + epsilon) * gain).astype(jnp.bfloat16)

    def attend(query, keys, vals, before):
        query = normed_rows(query, query_gain)
        zero = jnp.zeros_like(query)
        stacked = jnp.concatenate([jnp.where(head_of == h, query, zero) for h in range(local)], axis=0)
        scores = lax.dot_general(
            stacked, keys, (((1,), (1,)), ((), ())), preferred_element_type=jnp.float32
        ) * HK ** (-0.5)
        last = jnp.where(visible, scores[:, before:], -jnp.inf)
        scores = last if before == 0 else jnp.concatenate([scores[:, :before], last], axis=1)
        raised = jnp.exp(scores - jnp.max(scores, axis=1, keepdims=True))
        weights = (raised * (1.0 / jnp.sum(raised, axis=1, keepdims=True))).astype(jnp.bfloat16)
        return [
            jnp.dot(
                weights[h * rows : (h + 1) * rows], vals[:, h * HV : (h + 1) * HV],
                preferred_element_type=jnp.float32,
            ).astype(jnp.bfloat16)
            for h in range(local)
        ]

    def mix(pair_, maps):
        parts = []
        for h in range(local):
            mixed = maps[0][h].astype(jnp.float32) - lam_ref[pair_ * local + h] * maps[1][h].astype(jnp.float32)
            mean = jnp.mean(mixed * mixed, axis=1, keepdims=True)
            parts.append((mixed * lax.rsqrt(mean + epsilon) * sub_gain).astype(jnp.bfloat16))
        return jnp.concatenate(parts, axis=1)

    def new_keys(m, i):
        kn[m, i * rows : (i + 1) * rows, :] = normed_rows(kb[m, i * rows : (i + 1) * rows, :], key_gain)

    def pair_map(m, i):
        keys = (i + 1) * rows
        return attend(qb[m, i * rows : keys, :], kn[m, :keys, :], vb[:keys, :], i * rows)

    def near(z):
        keys = (z + 1) * rows
        for p in range(half_sp):
            maps = []
            for m in range(2):
                for i in range(z + 1):
                    knx[m, i * rows : (i + 1) * rows, :] = normed_rows(
                        kx[m, i * rows : (i + 1) * rows, p * width : (p + 1) * width], key_gain
                    )
                maps.append(attend(
                    qx[m, :, p * width : (p + 1) * width], knx[m, :keys, :],
                    vx[:keys, p * vwidth : (p + 1) * vwidth], z * rows,
                ))
            nbuf[half_sp + p] = mix(half_sp + p, maps)

    def give(z, i, maps):
        if i == z:
            nbuf[z] = mix(z, maps)
        else:
            nsend[i] = mix(z, maps)
            back(z, i).start()

    def below(z):
        for copy in rows_in(z):
            copy.wait()
        if z == 1:
            for held, sent, m in relays:
                move(0, 1, held, m).wait_recv()
                for o in highs:
                    move(1, o, sent, m).start()
        weights_first()
        near(z)
        for i in range(sp):
            maps = []
            for m in range(2):
                if i != z:
                    for f in five[3 * m : 3 + 2 * m]:
                        move(i, z, *f).wait_recv()
                new_keys(m, i)
                maps.append(pair_map(m, i))
            give(z, i, maps)
            if i == half_sp:
                weights_next()

    def above(z):
        for copy in rows_in(z):
            copy.wait()
        weights_first()
        weights_next()
        other = half_sp + sp - 1 - z
        both = {i: [] for i in highs}
        for m in range(2):
            for f in five[3 * m : 3 + 2 * m]:
                move(other, z, *f).wait_recv()
                if f[0] != "q":
                    move(1, z, *f).wait_recv()
                    move(0 + 1, z, "r" + f[0], f[1]).wait_recv()
            for i in range(sp):
                new_keys(m, i)
            for i in (other, z):
                both[i].append(pair_map(m, i))
        for i in (other, z):
            give(z, i, both[i])

    for z in range(sp):
        @pl.when(me == z)
        def _(z=z):
            below(z) if z in lows else above(z)

    def gather_back(owners):
        for z in range(sp):
            @pl.when(me == z)
            def _(z=z):
                for o in owners:
                    if o != z and (o in lows or z in highs):
                        back(o, z).wait_recv()

    def project(shard, owners, first):
        normed = jnp.concatenate([nbuf[j] for j in owners], axis=1)
        weight = wbuf[shard, owners[0] * vwidth : (owners[-1] + 1) * vwidth, :]
        here = pl.ds(pl.multiple_of(shard * columns, 128), columns)
        total = jnp.dot(normed, weight, preferred_element_type=jnp.float32)
        if first:
            acc[:, here] = total
        else:
            out_ref[:, here] = (acc[:, here] + total).astype(jnp.bfloat16)

    weights_last()
    gather_back(highs)
    own_weights().wait()
    for c in range(chips):
        project(shard_of(d, c), highs, True)
    for c in range(chips):
        at_ = shard_of(partner, c)
        pltpu.make_async_remote_copy(
            src_ref=wbuf.at[at_], dst_ref=wbuf.at[at_], send_sem=p_send.at[c], recv_sem=p_recv.at[c],
            device_id=(me, partner), device_id_type=MESH,
        ).wait_recv()
        project(at_, highs, True)
    gather_back(lows)
    for c in range(chips):
        project(shard_of(d, c), lows, False)
        project(shard_of(partner, c), lows, False)

    for z in range(sp):
        @pl.when(me == z)
        def _(z=z):
            for key in outgoing(z):
                move(*key).wait_send()
            if z == 1:
                for _, sent, m in relays:
                    for o in highs:
                        move(1, o, sent, m).wait_send()
            for i in range(sp):
                if i != z and (z in lows or i in highs):
                    back(z, i).wait_send()
    for c in range(chips):
        pair(c).wait_send()
        if c:
            for h in range(2):
                spread(c, h).wait_send()


def fused(sp, dp, query_rows, key_rows, value_rows, lambdas, query_gain, key_gain, sub_gain, out_weight):
    rows = query_rows.shape[1]
    length = rows * sp
    local = HEADS // sp
    width, vwidth = local * HK, local * HV
    depth, columns = out_weight.shape
    vmem = pl.BlockSpec(memory_space=pltpu.VMEM)
    hbm = pl.BlockSpec(memory_space=pl.ANY)
    dma = pltpu.SemaphoreType.DMA
    out = pl.pallas_call(
        functools.partial(kernel, sp, dp),
        out_shape=pltpu.VMEM((rows, columns * dp), jnp.bfloat16),
        in_specs=[hbm] * 8,
        out_specs=vmem,
        scratch_shapes=[
            pltpu.VMEM((2, length, width), jnp.bfloat16),
            pltpu.VMEM((2, length, width), jnp.bfloat16),
            pltpu.VMEM((length, vwidth), jnp.bfloat16),
            pltpu.VMEM((2, length, width), jnp.bfloat16),
            pltpu.VMEM((2, rows, sp // 2 * width), jnp.bfloat16),
            pltpu.VMEM((2, sp // 2 * rows, sp // 2 * width), jnp.bfloat16),
            pltpu.VMEM((sp // 2 * rows, sp // 2 * vwidth), jnp.bfloat16),
            pltpu.VMEM((2, sp // 2 * rows, width), jnp.bfloat16),
            pltpu.VMEM((sp, rows, vwidth), jnp.bfloat16),
            pltpu.VMEM((sp, rows, vwidth), jnp.bfloat16),
            pltpu.VMEM((dp, depth, columns), jnp.bfloat16),
            dma((10,)), dma((5 * sp * sp,)), dma((5 * sp * sp,)), dma((sp,)), dma((sp,)),
            dma((dp // 2, 2)), dma((dp // 2, 2)), dma((dp // 2,)), dma((dp // 2,)), dma,
            pltpu.SMEM(lambdas.shape, jnp.float32),
            pltpu.VMEM((1, HK), jnp.float32), pltpu.VMEM((1, HK), jnp.float32), pltpu.VMEM((1, HV), jnp.float32),
            dma((4,)),
            pltpu.VMEM((rows, columns * dp), jnp.float32),
        ],
        compiler_params=pltpu.CompilerParams(collective_id=0, has_side_effects=True),
    )(
        query_rows[0], key_rows[0], value_rows[0], lambdas,
        query_gain[None], key_gain[None], sub_gain[None], out_weight,
    )
    return out[None]


def solution(mesh):
    in_specs = (
        P("dp", "sp", None),
        P("dp", "sp", None),
        P("dp", "sp", None),
        P(),
        P(),
        P(),
        P(),
        P(None, "dp"),
    )
    out_specs = P("dp", "sp", None)
    sp, dp = mesh.shape["sp"], mesh.shape["dp"]

    def step(*operands):
        if fits(sp, dp, operands[0].shape, operands[7].shape):
            return fused(sp, dp, *operands)
        return body(*operands)

    return jax.shard_map(step, mesh=mesh, in_specs=in_specs, out_specs=out_specs, check_vma=False)
```
